256 devices in a mesh: st: 16 (over y, x), tp: 16 (over z, core).
Axes of the slice: x: 4, y: 4, z: 8, core: 2. Of those that a mesh axis runs over, the one named last changes fastest.
Arguments:
- normed: bfloat16 [8192, 2048], P('st'), may hold values from -128 to 128
- store: bfloat16 [32768, 2048], P('st'), may hold values from -5 to 5
- passage_ids: int32 [64, 2], P('st'), may hold values from 0 to 511, as said below
- w_query: bfloat16 [2048, 2048], P(None, 'tp'), as said below
- w_gate: bfloat16 [2048, 2048], P(None, 'tp'), may hold values from -0.125 to 0.125
- w_key: bfloat16 [2048, 2048], P(None, 'tp'), as said below
- w_value: bfloat16 [2048, 2048], P(None, 'tp'), may hold values from -0.125 to 0.125
- cotangent: bfloat16 [8192, 2048], P('st', 'tp'), may hold values from -6 to 6
Outputs:
- grad_rows: float32 [8192, 2048], P('st', 'tp')
- grad_store: float32 [32768, 2048], P('st', 'tp')
- grad_query_weight: float32 [2048, 2048], P('st', 'tp')
The draws below stay inside these ranges and needn't reach their ends.
Inputs may be any that keep to these rules, and one draw needn't show every extreme that they name: `passage_ids`: each row names 2 passages. The passages read by the blocks of one index of st are all different, and at most 1 of them belong to any one owner (the owner of passage p is the index p // 32 of st). In every draw some owner has one of its passages read by every index of st. `w_query`: entries lie within 6 * 2048 ** -0.5 in magnitude. `w_key`: entries lie within 8 * 2048 ** -0.5 in magnitude.
All inputs are finite; a program needn't handle non-finite values.
Results may differ from the reference program's by a relative error of at most 0.019.
Values may be sent and summed in bfloat16 or wider, within the bound.
No kernel may reach another device: no remote copies, remote signals or barrier semaphores. Data moves between devices by JAX's collectives and lax.ppermute only.
A program may use at most 128 MiB of HBM per device.

```python
import jax
import jax.numpy as jnp
from jax import lax

D = 2048
DH = 128
BLK = 128
R = 2
PLEN = 64
TOK_DEV = 512
PASS_DEV = 32
TOKENS = 8192
NPASS = 512
STORE_ROWS = 32768


def request_table(key):
    base = jax.random.fold_in(key, 11)
    owners_count = NPASS // PASS_DEV
    requests = TOK_DEV // BLK * R
    slot_most = max(1, 2 * requests // owners_count)
    slot_count = owners_count * slot_most
    subkeys = jax.random.split(base, 5)
    popular = jax.random.randint(subkeys[0], (owners_count,), 0, 2)
    hottest = jax.random.randint(subkeys[1], (), 0, owners_count)
    device = jnp.arange(owners_count, dtype=jnp.int32)[:, None]
    slot_ids = jnp.arange(slot_count, dtype=jnp.int32)[None, :]
    slot_owner = slot_ids // slot_most
    slot_rank = slot_ids % slot_most
    previous = (device - 1) % owners_count
    opposite = (device + owners_count // 2) % owners_count
    forced = ((slot_owner == hottest) | (slot_owner == previous)).astype(jnp.int32)
    halfway = ((slot_owner == opposite) & (slot_rank == 0)).astype(jnp.int32)
    leading = ((slot_owner == previous) & (slot_rank == 0)).astype(jnp.int32)
    tier = popular[slot_owner] + 3 * forced + 2 * halfway + 8 * leading
    noise = jax.random.randint(subkeys[2], (owners_count, slot_count), 0, 65536)
    score = (tier * 65536 + noise) * slot_count + slot_ids
    chosen = jnp.argsort(-score, axis=1)[:, :requests]
    chosen_owner = chosen // slot_most
    picks = jax.random.randint(subkeys[3], (owners_count, owners_count), 0, PASS_DEV)
    picks = picks.at[0, owners_count - 1].set(PASS_DEV - 1)
    picks = picks.at[1 % owners_count, 0].set(0)
    first_pick = jnp.take_along_axis(picks, chosen_owner, axis=1)
    local_ids = (first_pick + chosen % slot_most) % PASS_DEV
    passage = chosen_owner * PASS_DEV + local_ids
    shuffle = jax.random.randint(subkeys[4], (owners_count, requests), 0, 1 << 20) * requests
    shuffle = shuffle + jnp.arange(requests, dtype=jnp.int32)[None, :]
    arrangement = jnp.argsort(shuffle, axis=1)
    passage = jnp.take_along_axis(passage, arrangement, axis=1)
    return passage.reshape(-1, R).astype(jnp.int32)


def store_values(key):
    return jnp.clip(jax.random.normal(jax.random.fold_in(key, 21), (STORE_ROWS, D), jnp.float32), -5.0, 5.0)


def query_weight(key):
    fresh = jax.random.normal(jax.random.fold_in(key, 31), (D, D), jnp.float32)
    return jnp.clip(fresh, -6.0, 6.0) * D ** (-0.5)


def draw_passage_ids(key, part):
    return request_table(key)


def draw_store(key, part):
    return store_values(key).astype(jnp.bfloat16)


def draw_w_query(key, part):
    return query_weight(key).astype(jnp.bfloat16)


def draw_w_key(key, part):
    fresh = jnp.clip(jax.random.normal(jax.random.fold_in(key, 41), (D, D), jnp.float32), -6.0, 6.0) * D ** (-0.5)
    return fresh.astype(jnp.bfloat16)


def draw_normed(key, part):
    rows = jnp.clip(jax.random.normal(jax.random.fold_in(key, 51), (TOKENS, D), jnp.float32), -6.0, 6.0)
    return rows.astype(jnp.bfloat16)


def level_of(own_key, dims, pieces, low, largest):
    gain = 1.0
    for axis_at, parts in pieces:
        heights = jax.random.uniform(jax.random.fold_in(jax.random.fold_in(own_key, 6), axis_at), (parts,), jnp.float32, low / len(pieces), largest / len(pieces))
        gain = gain * jnp.repeat(jnp.exp(heights), dims[axis_at] // parts).reshape((-1,) + (1,) * (len(dims) - 1 - axis_at))
    return gain


def bell_draw(stream_key, dims, scale, bound, shards=(), kind=jnp.bfloat16):
    entries = jax.random.normal(stream_key, dims, jnp.float32) * scale
    if len(shards) > 0:
        entries = level_of(stream_key, dims, shards, -0.22, 0.18) * entries
    return jnp.clip(entries, min=-bound, max=bound).astype(kind)


def setup_inputs(seed: int = 0) -> dict:
    seeds = jax.random.split(jax.random.key(seed), 9)
    normed = draw_normed(jax.random.fold_in(seeds[8], 71), 0)
    store = draw_store(jax.random.fold_in(seeds[8], 71), 0)
    passage_ids = draw_passage_ids(jax.random.fold_in(seeds[8], 71), 0)
    w_query = draw_w_query(jax.random.fold_in(seeds[8], 71), 0)
    w_gate = bell_draw(seeds[4], (D, D), D ** -0.5, 0.125, ((1, 16),))
    w_key = draw_w_key(jax.random.fold_in(seeds[8], 71), 0)
    w_value = bell_draw(seeds[6], (D, D), D ** -0.5, 0.125, ((1, 16),))
    cotangent = bell_draw(seeds[7], (TOKENS, D), 1.0, 6.0, ((0, 16), (1, 16)))
    return dict(normed=normed, store=store, passage_ids=passage_ids, w_query=w_query, w_gate=w_gate, w_key=w_key, w_value=w_value, cotangent=cotangent)


def reference(normed, store, passage_ids, w_query, w_gate, w_key, w_value, cotangent):
    tokens, model_width = normed.shape
    blocks = tokens // BLK
    heads = model_width // DH
    score_scale = DH ** -0.5
    queries = jnp.dot(normed, w_query, preferred_element_type=jnp.float32).astype(jnp.bfloat16)
    gate_open = jax.nn.sigmoid(jnp.dot(normed, w_gate, preferred_element_type=jnp.float32))
    key_all = jnp.dot(store, w_key, preferred_element_type=jnp.float32).astype(jnp.bfloat16)
    value_all = jnp.dot(store, w_value, preferred_element_type=jnp.float32).astype(jnp.bfloat16)
    key_all = key_all.reshape(NPASS, PLEN, heads, DH)
    value_all = value_all.reshape(NPASS, PLEN, heads, DH)
    flat_ids = passage_ids.reshape(-1).astype(jnp.int32)
    key_rows = jnp.take(key_all, flat_ids, axis=0).reshape(blocks, R * PLEN, heads, DH).astype(jnp.float32)
    value_rows = jnp.take(value_all, flat_ids, axis=0).reshape(blocks, R * PLEN, heads, DH).astype(jnp.float32)
    q_blocks = queries.reshape(blocks, BLK, heads, DH).astype(jnp.float32)
    scores = jnp.einsum("bthd,bshd->bhts", q_blocks, key_rows) * score_scale
    attn_probs = jax.nn.softmax(scores, axis=-1)
    probs_low = attn_probs.astype(jnp.bfloat16).astype(jnp.float32)
    attended = jnp.einsum("bhts,bshd->bthd", probs_low, value_rows)
    gate_blocks = gate_open.reshape(blocks, BLK, heads, DH)
    upstream = cotangent.astype(jnp.float32).reshape(blocks, BLK, heads, DH)
    d_attended = (upstream * gate_blocks).astype(jnp.bfloat16).astype(jnp.float32)
    d_gate = (upstream * attended * gate_blocks * (1.0 - gate_blocks)).astype(jnp.bfloat16)
    d_values = jnp.einsum("bhts,bthd->bshd", probs_low, d_attended).astype(jnp.bfloat16)
    d_probs = jnp.einsum("bthd,bshd->bhts", d_attended, value_rows)
    row_delta = jnp.sum(d_probs * attn_probs, axis=-1, keepdims=True)
    d_scores = (attn_probs * (d_probs - row_delta) * score_scale).astype(jnp.bfloat16).astype(jnp.float32)
    d_query = jnp.einsum("bhts,bshd->bthd", d_scores, key_rows).astype(jnp.bfloat16).reshape(tokens, model_width)
    d_keys = jnp.einsum("bhts,bthd->bshd", d_scores, q_blocks).astype(jnp.bfloat16)
    grad_rows = jnp.dot(d_query, w_query.T, preferred_element_type=jnp.float32)
    grad_rows = grad_rows + jnp.dot(d_gate.reshape(tokens, model_width), w_gate.T, preferred_element_type=jnp.float32)
    reads_keys = d_keys.reshape(blocks * R, PLEN, model_width).astype(jnp.float32)
    reads_values = d_values.reshape(blocks * R, PLEN, model_width).astype(jnp.float32)
    summed_keys = jnp.zeros((NPASS, PLEN, model_width), jnp.float32).at[flat_ids].add(reads_keys)
    summed_values = jnp.zeros((NPASS, PLEN, model_width), jnp.float32).at[flat_ids].add(reads_values)
    grad_store = jnp.dot(summed_keys.reshape(NPASS * PLEN, model_width), w_key.astype(jnp.float32).T,
                         precision=lax.Precision.HIGHEST)
    grad_store = grad_store + jnp.dot(summed_values.reshape(NPASS * PLEN, model_width),
                                      w_value.astype(jnp.float32).T, precision=lax.Precision.HIGHEST)
    grad_query_weight = jnp.dot(normed.T, d_query, preferred_element_type=jnp.float32)
    return grad_rows, grad_store, grad_query_weight
```

```python
import functools

import jax
import jax.numpy as jnp
from jax import lax
from jax.experimental import pallas as pl
from jax.experimental.pallas import tpu as pltpu
from jax.sharding import PartitionSpec as P

DH = 128
BLK = 128
PLEN = 64
BF16 = jnp.bfloat16
F32 = jnp.float32

VMEM = pl.BlockSpec(memory_space=pltpu.VMEM)
SMEM = pl.BlockSpec(memory_space=pltpu.SMEM)


def nt(a, b):
    return lax.dot_general(a, b, (((1,), (1,)), ((), ())), preferred_element_type=F32)


def tn(a, b):
    return lax.dot_general(a, b, (((0,), (0,)), ((), ())), preferred_element_type=F32)


def nn(a, b):
    return lax.dot_general(a, b, (((1,), (0,)), ((), ())), preferred_element_type=F32)


def cost(flops, nbytes):
    return pl.CostEstimate(flops=flops, bytes_accessed=nbytes, transcendentals=0)


def project_body(x_ref, wa_ref, wb_ref, out_ref):
    pair = jnp.concatenate([wa_ref[...], wb_ref[...]], axis=1)
    out_ref[...] = nn(x_ref[...], pair).astype(BF16)


def project_rows(store, w_key, w_value, tile):
    rows, width = store.shape
    cols = w_key.shape[1]
    return pl.pallas_call(
        project_body,
        grid=(rows // tile,),
        in_specs=[
            pl.BlockSpec((tile, width), lambda i: (i, 0)),
            pl.BlockSpec((width, cols), lambda i: (0, 0)),
            pl.BlockSpec((width, cols), lambda i: (0, 0)),
        ],
        out_specs=pl.BlockSpec((tile, 2 * cols), lambda i: (i, 0)),
        out_shape=jax.ShapeDtypeStruct((rows, 2 * cols), BF16),
        cost_estimate=cost(4 * rows * width * cols, 2 * rows * width),
        name="project_store",
    )(store, w_key, w_value)


def query_body(x_ref, wa_ref, wb_ref, q_ref, g_ref):
    cols = wa_ref.shape[1]
    pair = jnp.concatenate([wa_ref[...], wb_ref[...]], axis=1)
    both = nn(x_ref[...], pair)
    q_ref[...] = both[:, :cols].astype(BF16)
    g_ref[...] = jax.nn.sigmoid(both[:, cols:])


def project_tokens(normed, w_query, w_gate, tile):
    rows, width = normed.shape
    cols = w_query.shape[1]
    return pl.pallas_call(
        query_body,
        grid=(rows // tile,),
        in_specs=[
            pl.BlockSpec((tile, width), lambda i: (i, 0)),
            pl.BlockSpec((width, cols), lambda i: (0, 0)),
            pl.BlockSpec((width, cols), lambda i: (0, 0)),
        ],
        out_specs=[pl.BlockSpec((tile, cols), lambda i: (i, 0))] * 2,
        out_shape=[
            jax.ShapeDtypeStruct((rows, cols), BF16),
            jax.ShapeDtypeStruct((rows, cols), F32),
        ],
        cost_estimate=cost(4 * rows * width * cols, 2 * rows * width),
        name="project_tokens",
    )(normed, w_query, w_gate)


def serve_body(wanted_ref, rows_ref, out_ref):
    for s in range(out_ref.shape[0]):
        out_ref[s] = rows_ref[jnp.maximum(wanted_ref[s], 0)]


def serve(wanted, projected):
    peers = wanted.shape[0]
    return pl.pallas_call(
        serve_body,
        in_specs=[SMEM, VMEM],
        out_specs=VMEM,
        out_shape=jax.ShapeDtypeStruct((peers,) + projected.shape[1:], BF16),
        cost_estimate=cost(1 << 20, 1 << 20),
        name="serve",
    )(wanted, projected)


def attend_body(owner_ref, q_ref, gate_ref, cot_ref, kv_ref, out_ref):
    scale = DH ** (-0.5)
    tokens = q_ref.shape[0]
    reads = BLK // PLEN
    for b in range(tokens // BLK):
        rows = slice(b * BLK, (b + 1) * BLK)
        kv = jnp.concatenate([kv_ref[owner_ref[reads * b + r]] for r in range(reads)], axis=0)
        keys, values = kv[:, :DH], kv[:, DH:]
        q = q_ref[rows, :]
        gate = gate_ref[rows, :]
        cot = cot_ref[rows, :].astype(F32)
        scores = nt(q, keys) * scale
        top = jnp.max(scores, axis=1, keepdims=True)
        grown = jnp.exp(scores - top)
        probs = grown / jnp.sum(grown, axis=1, keepdims=True)
        low = probs.astype(BF16)
        attended = nn(low, values)
        d_att = (cot * gate).astype(BF16)
        d_gate = (cot * attended * gate * (1.0 - gate)).astype(BF16)
        d_probs = nt(d_att, values)
        delta = jnp.sum(d_probs * probs, axis=1, keepdims=True)
        d_scores = (probs * (d_probs - delta) * scale).astype(BF16)
        out_ref[rows, :DH] = nn(d_scores, keys).astype(BF16)
        out_ref[rows, DH:] = d_gate
        reads_at = slice(tokens + b * BLK, tokens + (b + 1) * BLK)
        out_ref[reads_at, :DH] = tn(d_scores, q).astype(BF16)
        out_ref[reads_at, DH:] = tn(low, d_att).astype(BF16)


def attend(owners, queries, gate_open, cotangent, arrived):
    tokens = queries.shape[0]
    return pl.pallas_call(
        attend_body,
        in_specs=[SMEM, VMEM, VMEM, VMEM, VMEM],
        out_specs=VMEM,
        out_shape=jax.ShapeDtypeStruct((2 * tokens, 2 * DH), BF16),
        cost_estimate=cost(14 * tokens * DH * DH, 1 << 20),
        name="attend",
    )(owners, queries, gate_open, cotangent, arrived)


def weight_grad_body(d_ref, x_ref, out_ref):
    d_query = d_ref[: x_ref.shape[0], :DH]
    flipped = d_query.astype(F32).T.astype(BF16)
    for j in range(out_ref.shape[0] // 2):
        both = nn(flipped, x_ref[:, 2 * j * DH : 2 * (j + 1) * DH]).astype(BF16)
        out_ref[2 * j] = both[:, :DH]
        out_ref[2 * j + 1] = both[:, DH:]


def weight_grad(grads, normed):
    tokens, width = normed.shape
    return pl.pallas_call(
        weight_grad_body,
        in_specs=[VMEM, VMEM],
        out_specs=VMEM,
        out_shape=jax.ShapeDtypeStruct((width // DH, DH, DH), BF16),
        cost_estimate=cost(2 * tokens * width * DH, 2 * tokens * width),
        name="weight_grad",
    )(grads, normed)


def spread_body(steps, chips, mine_ref, other_ref, *refs):
    weights, outs = refs[:8], refs[8:]
    at = lax.axis_index("tp")
    core = lax.rem(at, 2)
    chip = lax.div(at, 2)
    tokens = mine_ref.shape[0] // 2
    for out_ref, step in zip(outs, steps):
        to = lax.rem(chip + step, chips) * 2 + core
        rows = pl.ds(pl.multiple_of(to * DH, DH), DH)
        part = [w[rows, :] for w in weights]
        for half in range(2):
            side = slice(half * tokens, (half + 1) * tokens)
            left = jnp.concatenate([mine_ref[side, :], other_ref[side, :]], axis=1)
            right = jnp.concatenate(
                [part[2 * half], part[2 * half + 1], part[4 + 2 * half], part[5 + 2 * half]], axis=1
            )
            out_ref[side, :] = nt(left, right).astype(BF16)


def spread(steps, chips, mine, other, weights):
    rows = mine.shape[0]
    return pl.pallas_call(
        functools.partial(spread_body, steps, chips),
        in_specs=[VMEM] * 10,
        out_specs=[VMEM] * len(steps),
        out_shape=[jax.ShapeDtypeStruct((rows, DH), BF16)] * len(steps),
        cost_estimate=cost(len(steps) * 8 * rows * DH * DH, 4 << 20),
        name="spread_" + "_".join(str(s) for s in steps),
    )(mine, other, *weights)


def finish_body(owner_ref, own_ref, left_ref, right_ref, rows_ref, slots_ref):
    tokens = rows_ref.shape[0]

    def total(at):
        return (
            own_ref[at, :].astype(F32) + left_ref[at, :].astype(F32) + right_ref[at, :].astype(F32)
        )

    rows_ref[...] = total(slice(0, tokens))
    slots_ref[...] = jnp.zeros_like(slots_ref)
    for i in range(tokens // PLEN):
        at = slice(tokens + i * PLEN, tokens + (i + 1) * PLEN)
        slots_ref[owner_ref[i]] = total(at).astype(BF16)


def finish(owners, own, left, right, peers):
    rows = own.shape[0]
    return pl.pallas_call(
        finish_body,
        in_specs=[SMEM, VMEM, VMEM, VMEM],
        out_specs=[VMEM, VMEM],
        out_shape=[
            jax.ShapeDtypeStruct((rows // 2, DH), F32),
            jax.ShapeDtypeStruct((peers, PLEN, DH), BF16),
        ],
        cost_estimate=cost(1 << 20, 1 << 20),
        name="finish",
    )(owners, own, left, right)


def collect_body(wanted_ref, returned_ref, out_ref):
    out_ref[...] = jnp.zeros_like(out_ref)
    for s in range(returned_ref.shape[0]):

        @pl.when(wanted_ref[s] >= 0)
        def _():
            at = jnp.maximum(wanted_ref[s], 0)
            out_ref[at] = out_ref[at] + returned_ref[s].astype(F32)


def collect(wanted, returned, passages):
    return pl.pallas_call(
        collect_body,
        in_specs=[SMEM, VMEM],
        out_specs=VMEM,
        out_shape=jax.ShapeDtypeStruct((passages, PLEN, DH), F32),
        cost_estimate=cost(1 << 20, 1 << 20),
        name="collect",
    )(wanted, returned)


def add_up_body(parts_ref, out_ref):
    out_ref[...] = jnp.sum(parts_ref[...].astype(F32), axis=0).T


def add_up(parts):
    return pl.pallas_call(
        add_up_body,
        in_specs=[VMEM],
        out_specs=VMEM,
        out_shape=jax.ShapeDtypeStruct(parts.shape[1:], F32),
        cost_estimate=cost(1 << 20, 1 << 20),
        name="add_up",
    )(parts)


def shards(normed, store, passage_ids, w_query, w_gate, w_key, w_value, cotangent):
    peers = lax.axis_size("st")
    members = lax.axis_size("tp")
    chips = members // 2
    pass_dev = store.shape[0] // PLEN
    flat_ids = passage_ids.reshape(-1)
    owners = flat_ids // pass_dev
    local_ids = flat_ids % pass_dev
    slot_hit = owners[:, None] == jnp.arange(peers, dtype=jnp.int32)[None, :]
    slot_table = jnp.max(jnp.where(slot_hit, local_ids[:, None], -1), axis=0)
    wanted = lax.all_to_all(slot_table.reshape(peers, 1), "st", 0, 0, tiled=True).reshape(peers)

    partner = [(t, t ^ 1) for t in range(members)]
    mine = (w_query, w_gate, w_key, w_value)
    theirs = tuple(lax.ppermute(w, "tp", partner) for w in mine)

    projected = project_rows(store, w_key, w_value, 256)
    served = serve(wanted, projected.reshape(pass_dev, PLEN, 2 * DH))
    arrived = lax.all_to_all(served, "st", 0, 0, tiled=True)
    queries, gate_open = project_tokens(normed, w_query, w_gate, 256)
    grads = attend(owners, queries, gate_open, cotangent, arrived)

    other = lax.ppermute(grads, "tp", partner)
    weight_parts = lax.all_to_all(weight_grad(grads, normed), "st", 0, 0, tiled=True)
    order = (4, 5, 3, 6, 2, 7, 1, 0)
    part = dict(zip(order, spread(order, chips, grads, other, mine + theirs)))

    def hop(array, by):
        return lax.ppermute(array, "tp", [(t, (t + 2 * by) % members) for t in range(members)])

    up = hop(part[4], 1)
    down = hop(part[5], -1)
    up = hop(part[3] + up, 1)
    down = hop(part[6] + down, -1)
    up = hop(part[2] + up, 1)
    down = hop(part[7] + down, -1)
    up = hop(part[1] + up, 1)
    grad_rows, outgoing = finish(owners, part[0], up, down, peers)
    returned = lax.all_to_all(outgoing, "st", 0, 0, tiled=True)
    grad_store = collect(wanted, returned, pass_dev).reshape(pass_dev * PLEN, DH)
    grad_query_weight = add_up(weight_parts)
    return (grad_rows, grad_store, grad_query_weight)


def solution(mesh):
    placed = (
        P("st", None),
        P("st", None),
        P("st", None),
        P(None, "tp"),
        P(None, "tp"),
        P(None, "tp"),
        P(None, "tp"),
        P("st", "tp"),
    )
    return jax.shard_map(
        shards,
        mesh=mesh,
        in_specs=placed,
        out_specs=(P("st", "tp"), P("st", "tp"), P("st", "tp")),
        check_vma=False,
    )
```

```python
import functools

import jax
import jax.numpy as jnp
from jax import lax
from jax.experimental import pallas as pl
from jax.experimental.pallas import tpu as pltpu
from jax.sharding import PartitionSpec as P


DH = 128
BLK = 128
PLEN = 64
BF16 = jnp.bfloat16
F32 = jnp.float32
NEAR = 40
TOKENS = 40
ATTEND = 8
SERVE = 61
GRAD = 40

VMEM = pl.BlockSpec(memory_space=pltpu.VMEM)
SMEM = pl.BlockSpec(memory_space=pltpu.SMEM)


def nt(a, b):
    return lax.dot_general(a, b, (((1,), (1,)), ((), ())), preferred_element_type=F32)


def tn(a, b):
    return lax.dot_general(a, b, (((0,), (0,)), ((), ())), preferred_element_type=F32)


def nn(a, b):
    return lax.dot_general(a, b, (((1,), (0,)), ((), ())), preferred_element_type=F32)


def grant(mib):
    return pltpu.CompilerParams(vmem_limit_bytes=mib << 20)


def cost(flops, nbytes):
    return pl.CostEstimate(flops=flops, bytes_accessed=nbytes, transcendentals=0)


def request_body(pass_dev, ids_ref, table_ref, owner_ref):
    reads, blocks = ids_ref.shape
    lanes = table_ref.shape[1:]
    table_ref[...] = jnp.full(table_ref.shape, -1, jnp.int32)
    for b in range(blocks):
        for r in range(reads):
            passage = ids_ref[r, b]
            owner = lax.div(passage, pass_dev)
            table_ref[owner] = jnp.full(lanes, passage - owner * pass_dev, jnp.int32)
            owner_ref[b * reads + r] = owner


def request(passage_ids, pass_dev, peers):
    return pl.pallas_call(
        functools.partial(request_body, pass_dev),
        in_specs=[SMEM],
        out_specs=[VMEM, SMEM],
        out_shape=[
            jax.ShapeDtypeStruct((peers, 1, 128), jnp.int32),
            jax.ShapeDtypeStruct((passage_ids.size,), jnp.int32),
        ],
        cost_estimate=cost(1 << 16, 1 << 16),
        name="request",
    )(passage_ids.T)


def project_body(x_ref, wa_ref, wb_ref, out_ref):
    pair = jnp.concatenate([wa_ref[...], wb_ref[...]], axis=1)
    out_ref[...] = nn(x_ref[...], pair).astype(BF16)


def project_rows(store, w_key, w_value, tile):
    rows, width = store.shape
    cols = w_key.shape[1]
    return pl.pallas_call(
        project_body,
        grid=(rows // tile,),
        in_specs=[
            pl.BlockSpec((tile, width), lambda i: (i, 0)),
            pl.BlockSpec((width, cols), lambda i: (0, 0)),
            pl.BlockSpec((width, cols), lambda i: (0, 0)),
        ],
        out_specs=pl.BlockSpec((tile, 2 * cols), lambda i: (i, 0)),
        out_shape=jax.ShapeDtypeStruct((rows, 2 * cols), BF16),
        cost_estimate=cost(4 * rows * width * cols, 2 * rows * width),
        name="project_store",
    )(store, w_key, w_value)


def serve_body(wanted_ref, rows_ref, out_ref, kept_ref):
    last = rows_ref.shape[0] - 1
    for s in range(out_ref.shape[0]):
        kept_ref[s] = wanted_ref[s, 0, 0]
        out_ref[s] = rows_ref[jnp.clip(wanted_ref[s, 0, 0], 0, last)]


def serve(wanted, projected):
    peers = wanted.shape[0]
    return pl.pallas_call(
        serve_body,
        in_specs=[SMEM, VMEM],
        out_specs=[VMEM, SMEM],
        out_shape=[
            jax.ShapeDtypeStruct((peers,) + projected.shape[1:], BF16),
            jax.ShapeDtypeStruct((peers,), jnp.int32),
        ],
        compiler_params=grant(SERVE),
        cost_estimate=cost(1 << 20, 2 << 20),
        name="serve",
    )(wanted, projected)


def query_body(x_ref, wa_ref, wb_ref, cot_ref, q_ref, up_ref, slope_ref):
    cols = wa_ref.shape[1]
    pair = jnp.concatenate([wa_ref[...], wb_ref[...]], axis=1)
    both = nn(x_ref[...], pair)
    q_ref[...] = both[:, :cols].astype(BF16)
    gate = jax.nn.sigmoid(both[:, cols:])
    up = cot_ref[...].astype(F32) * gate
    up_ref[...] = up.astype(BF16)
    slope_ref[...] = (up * (1.0 - gate)).astype(BF16)


def project_tokens(normed, w_query, w_gate, cotangent, tile):
    rows, width = normed.shape
    cols = w_query.shape[1]
    return pl.pallas_call(
        query_body,
        grid=(rows // tile,),
        in_specs=[
            pl.BlockSpec((tile, width), lambda i: (i, 0)),
            pl.BlockSpec((width, cols), lambda i: (0, 0)),
            pl.BlockSpec((width, cols), lambda i: (0, 0)),
            pl.BlockSpec((tile, cols), lambda i: (i, 0)),
        ],
        out_specs=[pl.BlockSpec((tile, cols), lambda i: (i, 0))] * 3,
        out_shape=[jax.ShapeDtypeStruct((rows, cols), BF16)] * 3,
        compiler_params=grant(TOKENS),
        cost_estimate=cost(4 * rows * width * cols, 2 * rows * width),
        name="project_tokens",
    )(normed, w_query, w_gate, cotangent)


def attend_body(owner_ref, q_ref, up_ref, slope_ref, kv_ref, out_ref):
    scale = DH ** (-0.5)
    tokens = q_ref.shape[0]
    reads = BLK // PLEN
    blocks = range(tokens // BLK)
    rows = [slice(b * BLK, (b + 1) * BLK) for b in blocks]
    kv = [
        jnp.concatenate([kv_ref[owner_ref[reads * b + r]] for r in range(reads)], axis=0)
        for b in blocks
    ]
    scores = [nt(q_ref[rows[b], :], kv[b][:, :DH]) * scale for b in blocks]
    d_att = [up_ref[rows[b], :] for b in blocks]
    d_probs = [nt(d_att[b], kv[b][:, DH:]) for b in blocks]
    grown = [jnp.exp(x - jnp.max(x, axis=1, keepdims=True)) for x in scores]
    probs = [x / jnp.sum(x, axis=1, keepdims=True) for x in grown]
    low = [x.astype(BF16) for x in probs]
    attended = [nn(low[b], kv[b][:, DH:]) for b in blocks]
    delta = [jnp.sum(d_probs[b] * probs[b], axis=1, keepdims=True) for b in blocks]
    d_scores = [(probs[b] * (d_probs[b] - delta[b]) * scale).astype(BF16) for b in blocks]
    for b in blocks:
        at = slice(tokens + b * BLK, tokens + (b + 1) * BLK)
        out_ref[at, DH:] = tn(low[b], d_att[b]).astype(BF16)
    for b in blocks:
        out_ref[rows[b], :DH] = nn(d_scores[b], kv[b][:, :DH]).astype(BF16)
    for b in blocks:
        out_ref[rows[b], DH:] = (slope_ref[rows[b], :].astype(F32) * attended[b]).astype(BF16)
    for b in blocks:
        at = slice(tokens + b * BLK, tokens + (b + 1) * BLK)
        out_ref[at, :DH] = tn(d_scores[b], q_ref[rows[b], :]).astype(BF16)


def attend(owners, queries, upstream, slope, arrived):
    tokens = queries.shape[0]
    return pl.pallas_call(
        attend_body,
        in_specs=[SMEM, VMEM, VMEM, VMEM, VMEM],
        out_specs=VMEM,
        out_shape=jax.ShapeDtypeStruct((2 * tokens, 2 * DH), BF16),
        cost_estimate=cost(14 * tokens * DH * DH, 1 << 20),
        compiler_params=grant(ATTEND),
        name="attend",
    )(owners, queries, upstream, slope, arrived)


def weight_grad_body(d_ref, x_ref, out_ref):
    d_query = d_ref[: x_ref.shape[0], :DH]
    flipped = d_query.astype(F32).T.astype(BF16)
    for j in range(out_ref.shape[0] // 2):
        both = nn(flipped, x_ref[:, 2 * j * DH : 2 * (j + 1) * DH]).astype(BF16)
        out_ref[2 * j] = both[:, :DH]
        out_ref[2 * j + 1] = both[:, DH:]


def weight_grad(grads, normed):
    tokens, width = normed.shape
    return pl.pallas_call(
        weight_grad_body,
        in_specs=[VMEM, VMEM],
        out_specs=VMEM,
        out_shape=jax.ShapeDtypeStruct((width // DH, DH, DH), BF16),
        compiler_params=grant(GRAD),
        cost_estimate=cost(2 * tokens * width * DH, 2 * tokens * width),
        name="weight_grad",
    )(grads, normed)


def both_heads(mine_ref, other_ref, side):
    return jnp.concatenate([mine_ref[side, :], other_ref[side, :]], axis=1)


def place(chips):
    at = lax.axis_index("tp")
    core = lax.rem(at, 2)
    chip = lax.div(at, 2)

    def first_row(k):
        to = lax.rem(chip + k + core * (chips - 2 * k), chips)
        return pl.multiple_of(to * 2 * DH, 2 * DH)

    return core, chip, first_row


JOBS = ((1, 3), (0, 3), (1, 2), (0, 2), (1, 1), (0, 1), (1, 0), (0, 0))


def pick_body(chips, *refs):
    weights, (far_ref, near_ref, far_sems, near_sems) = refs[:8], refs[8:]
    core, chip, first_row = place(chips)

    def source(half, piece):
        return weights[(2 * half, 2 * half + 1, 4 + 2 * half, 5 + 2 * half)[piece]]

    def far_copy(half, piece):
        return pltpu.make_async_copy(
            source(half, piece).at[pl.ds(first_row(chips // 2), 2 * DH), :],
            far_ref.at[:, pl.ds(piece * DH, DH)],
            far_sems.at[piece],
        )

    def near_copy(job, piece):
        half, k = JOBS[job]
        start = first_row(k) if k else pl.multiple_of((2 * chip + core) * DH, DH)
        count = 2 * DH if k else DH
        return pltpu.make_async_copy(
            source(half, piece).at[pl.ds(start, count), :],
            near_ref.at[job, pl.ds(0, count), pl.ds(piece * DH, DH)],
            near_sems.at[job, piece],
        )

    for half in range(2):

        @pl.when(core == half)
        def _():
            for piece in range(4):
                far_copy(half, piece).start()

    pairs = [(job, piece) for job in range(len(JOBS)) for piece in range(4)]
    for job, piece in pairs:
        near_copy(job, piece).start()
    for piece in range(4):
        far_copy(0, piece).wait()
    for job, piece in pairs:
        near_copy(job, piece).wait()


def pick(chips, weights):
    return pl.pallas_call(
        functools.partial(pick_body, chips),
        in_specs=[pl.BlockSpec(memory_space=pltpu.HBM)] * 8,
        out_specs=[VMEM] * 2,
        out_shape=[
            jax.ShapeDtypeStruct((2 * DH, 4 * DH), BF16),
            jax.ShapeDtypeStruct((len(JOBS), 2 * DH, 4 * DH), BF16),
        ],
        scratch_shapes=[pltpu.SemaphoreType.DMA((4,)), pltpu.SemaphoreType.DMA((len(JOBS), 4))],
        cost_estimate=cost(1 << 28, 6 << 20),
        name="pick",
    )(*weights)


def far_body(mine_ref, other_ref, weight_ref, out_ref):
    core = lax.rem(lax.axis_index("tp"), 2)
    tokens = out_ref.shape[0]
    side = pl.ds(pl.multiple_of(core * tokens, tokens), tokens)
    out_ref[...] = nt(both_heads(mine_ref, other_ref, side), weight_ref[...]).astype(BF16)


def far(mine, other, weight):
    tokens = mine.shape[0] // 2
    return pl.pallas_call(
        far_body,
        in_specs=[VMEM] * 3,
        out_specs=VMEM,
        out_shape=jax.ShapeDtypeStruct((tokens, 2 * DH), BF16),
        compiler_params=grant(8),
        cost_estimate=cost(16 * tokens * DH * DH, 1 << 20),
        name="far",
    )(mine, other, weight)


def near_body(mine_ref, other_ref, held_ref, *outs):
    tokens = mine_ref.shape[0] // 2
    left = [both_heads(mine_ref, other_ref, slice(h * tokens, (h + 1) * tokens)) for h in range(2)]
    for job, (half, k) in enumerate(JOBS):
        right = held_ref[job, : 2 * DH if k else DH, :]
        outs[job][...] = nt(left[half], right).astype(BF16)


def near(mine, other, held):
    tokens = mine.shape[0] // 2
    return pl.pallas_call(
        near_body,
        in_specs=[VMEM] * 3,
        out_specs=[VMEM] * len(JOBS),
        out_shape=[
            jax.ShapeDtypeStruct((tokens, 2 * DH if k else DH), BF16) for _, k in JOBS
        ],
        compiler_params=grant(NEAR),
        cost_estimate=cost(56 * 2 * tokens * DH * DH, 4 << 20),
        name="near",
    )(mine, other, held)


def join_body(chosen, own_ref, came_ref, out_ref):
    came = came_ref[...].astype(F32)
    if chosen is not None:
        core = lax.rem(lax.axis_index("tp"), 2)
        came = jnp.where(core == chosen, came, jnp.zeros_like(came))
    out_ref[...] = (own_ref[...].astype(F32) + came).astype(BF16)


def join(own, came, chosen=None):
    return pl.pallas_call(
        functools.partial(join_body, chosen),
        in_specs=[VMEM] * 2,
        out_specs=VMEM,
        out_shape=jax.ShapeDtypeStruct(own.shape, BF16),
        compiler_params=grant(4),
        cost_estimate=cost(1 << 20, 1 << 20),
    )(own, came)


def part_body(own_ref, came_ref, same_ref, cross_ref):
    both = own_ref[...].astype(F32) + came_ref[...].astype(F32)
    core = lax.rem(lax.axis_index("tp"), 2)
    same_ref[...] = jnp.where(core == 0, both[:, :DH], both[:, DH:]).astype(BF16)
    cross_ref[...] = jnp.where(core == 0, both[:, DH:], both[:, :DH]).astype(BF16)


def part(own, came):
    return pl.pallas_call(
        part_body,
        in_specs=[VMEM] * 2,
        out_specs=[VMEM] * 2,
        out_shape=[jax.ShapeDtypeStruct((own.shape[0], DH), BF16)] * 2,
        compiler_params=grant(4),
        cost_estimate=cost(1 << 20, 1 << 20),
    )(own, came)


def total(own_ref, ours_ref, theirs_ref, at):
    return own_ref[at, :].astype(F32) + ours_ref[at, :].astype(F32) + theirs_ref[at, :].astype(F32)


def finish_reads_body(owner_ref, own_ref, ours_ref, theirs_ref, slots_ref):
    slots_ref[...] = jnp.zeros_like(slots_ref)
    for i in range(own_ref.shape[0] // PLEN):
        at = slice(i * PLEN, (i + 1) * PLEN)
        slots_ref[owner_ref[i]] = total(own_ref, ours_ref, theirs_ref, at).astype(BF16)


def finish_reads(owners, own, ours, theirs, peers):
    return pl.pallas_call(
        finish_reads_body,
        in_specs=[SMEM, VMEM, VMEM, VMEM],
        out_specs=VMEM,
        out_shape=jax.ShapeDtypeStruct((peers, PLEN, DH), BF16),
        compiler_params=grant(8),
        cost_estimate=cost(1 << 20, 1 << 20),
        name="finish_reads",
    )(owners, own, ours, theirs)


def finish_rows_body(own_ref, ours_ref, theirs_ref, out_ref):
    out_ref[...] = total(own_ref, ours_ref, theirs_ref, slice(0, own_ref.shape[0]))


def finish_rows(own, ours, theirs):
    return pl.pallas_call(
        finish_rows_body,
        in_specs=[VMEM] * 3,
        out_specs=VMEM,
        out_shape=jax.ShapeDtypeStruct(own.shape, F32),
        compiler_params=grant(8),
        cost_estimate=cost(1 << 20, 1 << 20),
        name="finish_rows",
    )(own, ours, theirs)


def collect_body(wanted_ref, returned_ref, out_ref, sum_ref, sems):
    pieces = sems.shape[0]
    count = out_ref.shape[0] // pieces

    def leave(i):
        at = pl.ds(i * count, count)
        return pltpu.make_async_copy(sum_ref.at[at], out_ref.at[at], sems.at[i])

    for i in range(pieces):
        sum_ref[i * count : (i + 1) * count] = jnp.zeros((count,) + sum_ref.shape[1:], F32)
        for s in range(returned_ref.shape[0]):
            passage = wanted_ref[s]

            @pl.when((passage >= i * count) & (passage < (i + 1) * count))
            def _():
                at = jnp.clip(passage, i * count, (i + 1) * count - 1)
                sum_ref[at] = sum_ref[at] + returned_ref[s].astype(F32)

        leave(i).start()
    for i in range(pieces):
        leave(i).wait()


def collect(wanted, returned, passages):
    pieces = 4
    return pl.pallas_call(
        collect_body,
        in_specs=[SMEM, VMEM],
        out_specs=pl.BlockSpec(memory_space=pltpu.HBM),
        out_shape=jax.ShapeDtypeStruct((passages, PLEN, DH), F32),
        scratch_shapes=[pltpu.VMEM((passages, PLEN, DH), F32), pltpu.SemaphoreType.DMA((pieces,))],
        compiler_params=grant(8),
        cost_estimate=cost(1 << 20, 1 << 20),
        name="collect",
    )(wanted, returned)


def add_up_body(parts_ref, out_ref):
    out_ref[...] = jnp.sum(parts_ref[...].astype(F32), axis=0).T


def add_up(parts):
    return pl.pallas_call(
        add_up_body,
        in_specs=[VMEM],
        out_specs=VMEM,
        out_shape=jax.ShapeDtypeStruct(parts.shape[1:], F32),
        cost_estimate=cost(1 << 20, 1 << 20),
        compiler_params=grant(4),
        name="add_up",
    )(parts)


def shards(normed, store, passage_ids, w_query, w_gate, w_key, w_value, cotangent):
    peers = lax.axis_size("st")
    members = lax.axis_size("tp")
    chips = members // 2
    pass_dev = store.shape[0] // PLEN
    table, owners = request(passage_ids, pass_dev, peers)
    wanted = lax.all_to_all(table, "st", 0, 0, tiled=True)

    partner = [(t, t ^ 1) for t in range(members)]
    along = [(2 * z + c, 2 * ((z + 1 - 2 * c) % chips) + c) for z in range(chips) for c in range(2)]
    across = [(a, b ^ 1) for a, b in along]

    def move(array, pairs):
        return lax.ppermute(array, "tp", pairs)

    mine = (w_query, w_gate, w_key, w_value)
    weights = mine + tuple(move(w, partner) for w in mine)
    projected = project_rows(store, w_key, w_value, 1024).reshape(pass_dev, PLEN, 2 * DH)
    wanted, weights, projected = lax.optimization_barrier((wanted, weights, projected))
    served, wanted = serve(wanted, projected)
    served, later, normed_later = lax.optimization_barrier((served, weights, normed))
    arrived = lax.all_to_all(served, "st", 0, 0, tiled=True)
    queries, upstream, slope = project_tokens(normed_later, later[0], later[1], cotangent, 256)
    weight4, held = pick(chips, later)
    arrived, weight4 = lax.optimization_barrier((arrived, weight4))
    grads = attend(owners, queries, upstream, slope, arrived)

    other = move(grads, partner)
    opposite = move(far(grads, other, weight4), along)
    reads3, rows3, reads2, rows2, reads1, rows1, reads0, rows0 = near(grads, other, held)
    reads = move(join(reads3, opposite, 1), along)
    parts = weight_grad(grads, normed)
    parts = lax.all_to_all(parts, "st", 0, 0, tiled=True)
    rows = move(join(rows3, opposite, 0), along)
    reads = move(join(reads2, reads), along)
    rows = move(join(rows2, rows), along)
    same, cross = part(reads1, reads)
    outgoing = finish_reads(owners, reads0, move(same, along), move(cross, across), peers)
    same, cross = part(rows1, rows)
    grad_rows = finish_rows(rows0, move(same, along), move(cross, across))
    returned = lax.all_to_all(outgoing, "st", 0, 0, tiled=True)
    grad_store = collect(wanted, returned, pass_dev).reshape(pass_dev * PLEN, DH)
    grad_query_weight = add_up(parts)
    return (grad_rows, grad_store, grad_query_weight)


def solution(mesh):
    placed = (
        P("st", None),
        P("st", None),
        P("st", None),
        P(None, "tp"),
        P(None, "tp"),
        P(None, "tp"),
        P(None, "tp"),
        P("st", "tp"),
    )
    return jax.shard_map(
        shards,
        mesh=mesh,
        in_specs=placed,
        out_specs=(P("st", "tp"), P("st", "tp"), P("st", "tp")),
        check_vma=False,
    )
```

```python
import functools

import jax
import jax.numpy as jnp
from jax import lax
from jax.experimental import pallas as pl
from jax.experimental.pallas import tpu as pltpu
from jax.sharding import PartitionSpec as P


DH = 128
BLK = 128
PLEN = 64
BF16 = jnp.bfloat16
F32 = jnp.float32
NEAR = 40
FAR = 16
TOKENS = 40
ATTEND = 8
SERVE = 61
PROJECT = 61
GRAD = 40
PICK = 61

VMEM = pl.BlockSpec(memory_space=pltpu.VMEM)
SMEM = pl.BlockSpec(memory_space=pltpu.SMEM)


def nt(a, b):
    return lax.dot_general(a, b, (((1,), (1,)), ((), ())), preferred_element_type=F32)


def tn(a, b):
    return lax.dot_general(a, b, (((0,), (0,)), ((), ())), preferred_element_type=F32)


def nn(a, b):
    return lax.dot_general(a, b, (((1,), (0,)), ((), ())), preferred_element_type=F32)


def grant(mib):
    return pltpu.CompilerParams(vmem_limit_bytes=mib << 20)


def cost(flops, nbytes):
    return pl.CostEstimate(flops=flops, bytes_accessed=nbytes, transcendentals=0)


def request_body(pass_dev, ids_ref, table_ref, owner_ref):
    reads, blocks = ids_ref.shape
    lanes = table_ref.shape[1:]
    table_ref[...] = jnp.full(table_ref.shape, -1, jnp.int32)
    for b in range(blocks):
        for r in range(reads):
            passage = ids_ref[r, b]
            owner = lax.div(passage, pass_dev)
            table_ref[owner] = jnp.full(lanes, passage - owner * pass_dev, jnp.int32)
            owner_ref[b * reads + r] = owner


def request(passage_ids, pass_dev, peers):
    return pl.pallas_call(
        functools.partial(request_body, pass_dev),
        in_specs=[SMEM],
        out_specs=[VMEM, SMEM],
        out_shape=[
            jax.ShapeDtypeStruct((peers, 1, 128), jnp.int32),
            jax.ShapeDtypeStruct((passage_ids.size,), jnp.int32),
        ],
        cost_estimate=cost(1 << 16, 1 << 16),
        name="request",
    )(passage_ids.T)


def project_body(x_ref, wa_ref, wb_ref, out_ref):
    pair = jnp.concatenate([wa_ref[...], wb_ref[...]], axis=1)
    out_ref[...] = nn(x_ref[...], pair).astype(BF16)


def project_rows(store, w_key, w_value, tile):
    rows, width = store.shape
    cols = w_key.shape[1]
    return pl.pallas_call(
        project_body,
        grid=(rows // tile,),
        in_specs=[
            pl.BlockSpec((tile, width), lambda i: (i, 0)),
            pl.BlockSpec((width, cols), lambda i: (0, 0)),
            pl.BlockSpec((width, cols), lambda i: (0, 0)),
        ],
        out_specs=pl.BlockSpec((tile, 2 * cols), lambda i: (i, 0)),
        out_shape=jax.ShapeDtypeStruct((rows, 2 * cols), BF16),
        compiler_params=grant(PROJECT),
        cost_estimate=cost(4 * rows * width * cols, 2 * rows * width),
        name="project_store",
    )(store, w_key, w_value)


def serve_body(wanted_ref, rows_ref, out_ref, kept_ref):
    last = rows_ref.shape[0] - 1
    for s in range(out_ref.shape[0]):
        kept_ref[s] = wanted_ref[s, 0, 0]
        out_ref[s] = rows_ref[jnp.clip(wanted_ref[s, 0, 0], 0, last)]


def serve(wanted, projected):
    peers = wanted.shape[0]
    return pl.pallas_call(
        serve_body,
        in_specs=[SMEM, VMEM],
        out_specs=[VMEM, SMEM],
        out_shape=[
            jax.ShapeDtypeStruct((peers,) + projected.shape[1:], BF16),
            jax.ShapeDtypeStruct((peers,), jnp.int32),
        ],
        compiler_params=grant(SERVE),
        cost_estimate=cost(1 << 20, 2 << 20),
        name="serve",
    )(wanted, projected)


def query_body(x_ref, wa_ref, wb_ref, cot_ref, q_ref, up_ref, slope_ref):
    cols = wa_ref.shape[1]
    pair = jnp.concatenate([wa_ref[...], wb_ref[...]], axis=1)
    both = nn(x_ref[...], pair)
    q_ref[...] = both[:, :cols].astype(BF16)
    gate = jax.nn.sigmoid(both[:, cols:])
    up = cot_ref[...].astype(F32) * gate
    up_ref[...] = up.astype(BF16)
    slope_ref[...] = (up * (1.0 - gate)).astype(BF16)


def project_tokens(normed, w_query, w_gate, cotangent, tile):
    rows, width = normed.shape
    cols = w_query.shape[1]
    return pl.pallas_call(
        query_body,
        grid=(rows // tile,),
        in_specs=[
            pl.BlockSpec((tile, width), lambda i: (i, 0)),
            pl.BlockSpec((width, cols), lambda i: (0, 0)),
            pl.BlockSpec((width, cols), lambda i: (0, 0)),
            pl.BlockSpec((tile, cols), lambda i: (i, 0)),
        ],
        out_specs=[pl.BlockSpec((tile, cols), lambda i: (i, 0))] * 3,
        out_shape=[jax.ShapeDtypeStruct((rows, cols), BF16)] * 3,
        compiler_params=grant(TOKENS),
        cost_estimate=cost(4 * rows * width * cols, 2 * rows * width),
        name="project_tokens",
    )(normed, w_query, w_gate, cotangent)


def attend_body(owner_ref, q_ref, up_ref, slope_ref, kv_ref, out_ref):
    scale = DH ** (-0.5)
    tokens = q_ref.shape[0]
    reads = BLK // PLEN
    blocks = range(tokens // BLK)
    rows = [slice(b * BLK, (b + 1) * BLK) for b in blocks]
    kv = [
        jnp.concatenate([kv_ref[owner_ref[reads * b + r]] for r in range(reads)], axis=0)
        for b in blocks
    ]
    scores = [nt(q_ref[rows[b], :], kv[b][:, :DH]) * scale for b in blocks]
    d_att = [up_ref[rows[b], :] for b in blocks]
    d_probs = [nt(d_att[b], kv[b][:, DH:]) for b in blocks]
    grown = [jnp.exp(x - jnp.max(x, axis=1, keepdims=True)) for x in scores]
    probs = [x / jnp.sum(x, axis=1, keepdims=True) for x in grown]
    low = [x.astype(BF16) for x in probs]
    attended = [nn(low[b], kv[b][:, DH:]) for b in blocks]
    delta = [jnp.sum(d_probs[b] * probs[b], axis=1, keepdims=True) for b in blocks]
    d_scores = [(probs[b] * (d_probs[b] - delta[b]) * scale).astype(BF16) for b in blocks]
    for b in blocks:
        at = slice(tokens + b * BLK, tokens + (b + 1) * BLK)
        out_ref[at, DH:] = tn(low[b], d_att[b]).astype(BF16)
    for b in blocks:
        out_ref[rows[b], :DH] = nn(d_scores[b], kv[b][:, :DH]).astype(BF16)
    for b in blocks:
        out_ref[rows[b], DH:] = (slope_ref[rows[b], :].astype(F32) * attended[b]).astype(BF16)
    for b in blocks:
        at = slice(tokens + b * BLK, tokens + (b + 1) * BLK)
        out_ref[at, :DH] = tn(d_scores[b], q_ref[rows[b], :]).astype(BF16)


def attend(owners, queries, upstream, slope, arrived):
    tokens = queries.shape[0]
    return pl.pallas_call(
        attend_body,
        in_specs=[SMEM, VMEM, VMEM, VMEM, VMEM],
        out_specs=VMEM,
        out_shape=jax.ShapeDtypeStruct((2 * tokens, 2 * DH), BF16),
        cost_estimate=cost(14 * tokens * DH * DH, 1 << 20),
        compiler_params=grant(ATTEND),
        name="attend",
    )(owners, queries, upstream, slope, arrived)


def weight_grad_body(d_ref, x_ref, out_ref):
    flipped = d_ref[: x_ref.shape[0], :DH].astype(F32).T.astype(BF16)
    for j in range(out_ref.shape[0] // 2):
        both = nn(flipped, x_ref[:, 2 * j * DH : 2 * (j + 1) * DH]).astype(BF16)
        out_ref[2 * j] = both[:, :DH]
        out_ref[2 * j + 1] = both[:, DH:]


def weight_grad(grads, normed):
    tokens, width = normed.shape
    return pl.pallas_call(
        weight_grad_body,
        in_specs=[VMEM, VMEM],
        out_specs=VMEM,
        out_shape=jax.ShapeDtypeStruct((width // DH, DH, DH), BF16),
        compiler_params=grant(GRAD),
        cost_estimate=cost(2 * tokens * width * DH, 2 * tokens * width),
        name="weight_grad",
    )(grads, normed)


def both_heads(mine_ref, other_ref, side):
    return jnp.concatenate([mine_ref[side, :], other_ref[side, :]], axis=1)


def first_row(chip, core, k, chips):
    to = lax.rem(chip + k + core * (chips - 2 * k), chips)
    return pl.multiple_of(to * 2 * DH, 2 * DH)


FIRST = ((None, 4), (1, 3), (0, 3))
REST = ((1, 2), (0, 2), (1, 1), (0, 1), (1, 0), (0, 0))


def pick_body(chips, *refs):
    weights, outs, sems = refs[:4], refs[4:8], refs[8:]
    at = lax.axis_index("tp")
    here = lax.rem(at, 2)
    chip = lax.div(at, 2)
    jobs = [(n, job) for n, table in enumerate((FIRST, REST)) for job in range(len(table))]

    def copy(n, job, who, piece, half):
        k = (FIRST, REST)[n][job][1]
        core = here if who == 0 else 1 - here
        home = pl.multiple_of((2 * chip + core) * DH, DH)
        start, count = (first_row(chip, core, k, chips), 2 * DH) if k else (home, DH)
        return pltpu.make_async_copy(
            weights[2 * half + piece].at[pl.ds(start, count), :],
            outs[2 * n + who].at[job, pl.ds(0, count), pl.ds(piece * DH, DH)],
            sems[n].at[who, piece, job],
        )

    for n, job in jobs:
        for who in range(2):
            for piece in range(2):
                half = (FIRST, REST)[n][job][0]
                if half is not None:
                    copy(n, job, who, piece, half).start()
                    continue
                for half in range(2):

                    @pl.when(here == (half if who == 0 else 1 - half))
                    def _():
                        copy(n, job, who, piece, half).start()

    for n, job in jobs:
        for who in range(2):
            for piece in range(2):
                copy(n, job, who, piece, 0).wait()


def pick(chips, weights):
    shapes = [
        jax.ShapeDtypeStruct((len(table), 2 * DH, 2 * DH), BF16) for table in (FIRST, REST)
    ]
    return pl.pallas_call(
        functools.partial(pick_body, chips),
        in_specs=[pl.BlockSpec(memory_space=pltpu.HBM)] * 4,
        out_specs=[VMEM] * 4,
        out_shape=[shapes[0], shapes[0], shapes[1], shapes[1]],
        scratch_shapes=[pltpu.SemaphoreType.DMA((2, 2, len(table))) for table in (FIRST, REST)],
        compiler_params=grant(PICK),
        cost_estimate=cost(1 << 28, 6 << 20),
        name="pick",
    )(*weights)


def spread_body(table, mine_ref, other_ref, held_ref, lent_ref, *outs):
    core = lax.rem(lax.axis_index("tp"), 2)
    tokens = mine_ref.shape[0] // 2
    for job, (half, k) in enumerate(table):
        start = core * tokens if half is None else half * tokens
        side = pl.ds(pl.multiple_of(start, tokens), tokens)
        count = 2 * DH if k else DH
        right = jnp.concatenate([held_ref[job, :count, :], lent_ref[job, :count, :]], axis=1)
        outs[job][...] = nt(both_heads(mine_ref, other_ref, side), right).astype(BF16)


def spread(table, mine, other, held, lent, mib):
    tokens = mine.shape[0] // 2
    return pl.pallas_call(
        functools.partial(spread_body, table),
        in_specs=[VMEM] * 4,
        out_specs=[VMEM] * len(table),
        out_shape=[
            jax.ShapeDtypeStruct((tokens, 2 * DH if k else DH), BF16) for _, k in table
        ],
        compiler_params=grant(mib),
        cost_estimate=cost(16 * len(table) * tokens * DH * DH, 2 << 20),
    )(mine, other, held, lent)


def join_body(chosen, own_ref, came_ref, out_ref):
    came = came_ref[...].astype(F32)
    if chosen is not None:
        core = lax.rem(lax.axis_index("tp"), 2)
        came = jnp.where(core == chosen, came, jnp.zeros_like(came))
    out_ref[...] = (own_ref[...].astype(F32) + came).astype(BF16)


def join(own, came, chosen=None):
    return pl.pallas_call(
        functools.partial(join_body, chosen),
        in_specs=[VMEM] * 2,
        out_specs=VMEM,
        out_shape=jax.ShapeDtypeStruct(own.shape, BF16),
        compiler_params=grant(4),
        cost_estimate=cost(1 << 20, 1 << 20),
    )(own, came)


def part_body(own_ref, came_ref, same_ref, cross_ref):
    both = own_ref[...].astype(F32) + came_ref[...].astype(F32)
    core = lax.rem(lax.axis_index("tp"), 2)
    same_ref[...] = jnp.where(core == 0, both[:, :DH], both[:, DH:]).astype(BF16)
    cross_ref[...] = jnp.where(core == 0, both[:, DH:], both[:, :DH]).astype(BF16)


def part(own, came):
    return pl.pallas_call(
        part_body,
        in_specs=[VMEM] * 2,
        out_specs=[VMEM] * 2,
        out_shape=[jax.ShapeDtypeStruct((own.shape[0], DH), BF16)] * 2,
        compiler_params=grant(4),
        cost_estimate=cost(1 << 20, 1 << 20),
    )(own, came)


def total(own_ref, ours_ref, theirs_ref, at):
    return own_ref[at, :].astype(F32) + ours_ref[at, :].astype(F32) + theirs_ref[at, :].astype(F32)


def finish_reads_body(owner_ref, own_ref, ours_ref, theirs_ref, slots_ref):
    slots_ref[...] = jnp.zeros_like(slots_ref)
    for i in range(own_ref.shape[0] // PLEN):
        at = slice(i * PLEN, (i + 1) * PLEN)
        slots_ref[owner_ref[i]] = total(own_ref, ours_ref, theirs_ref, at).astype(BF16)


def finish_reads(owners, own, ours, theirs, peers):
    return pl.pallas_call(
        finish_reads_body,
        in_specs=[SMEM, VMEM, VMEM, VMEM],
        out_specs=VMEM,
        out_shape=jax.ShapeDtypeStruct((peers, PLEN, DH), BF16),
        compiler_params=grant(8),
        cost_estimate=cost(1 << 20, 1 << 20),
        name="finish_reads",
    )(owners, own, ours, theirs)


def finish_rows_body(own_ref, ours_ref, theirs_ref, out_ref):
    out_ref[...] = total(own_ref, ours_ref, theirs_ref, slice(0, own_ref.shape[0]))


def finish_rows(own, ours, theirs):
    return pl.pallas_call(
        finish_rows_body,
        in_specs=[VMEM] * 3,
        out_specs=VMEM,
        out_shape=jax.ShapeDtypeStruct(own.shape, F32),
        compiler_params=grant(8),
        cost_estimate=cost(1 << 20, 1 << 20),
        name="finish_rows",
    )(own, ours, theirs)


def collect_body(wanted_ref, returned_ref, out_ref, sum_ref, sems):
    pieces = sems.shape[0]
    count = out_ref.shape[0] // pieces

    def leave(i):
        at = pl.ds(i * count, count)
        return pltpu.make_async_copy(sum_ref.at[at], out_ref.at[at], sems.at[i])

    for i in range(pieces):
        sum_ref[i * count : (i + 1) * count] = jnp.zeros((count,) + sum_ref.shape[1:], F32)
        for s in range(returned_ref.shape[0]):
            passage = wanted_ref[s]

            @pl.when((passage >= i * count) & (passage < (i + 1) * count))
            def _():
                at = jnp.clip(passage, i * count, (i + 1) * count - 1)
                sum_ref[at] = sum_ref[at] + returned_ref[s].astype(F32)

        leave(i).start()
    for i in range(pieces):
        leave(i).wait()


def collect(wanted, returned, passages):
    pieces = 4
    return pl.pallas_call(
        collect_body,
        in_specs=[SMEM, VMEM],
        out_specs=pl.BlockSpec(memory_space=pltpu.HBM),
        out_shape=jax.ShapeDtypeStruct((passages, PLEN, DH), F32),
        scratch_shapes=[pltpu.VMEM((passages, PLEN, DH), F32), pltpu.SemaphoreType.DMA((pieces,))],
        compiler_params=grant(8),
        cost_estimate=cost(1 << 20, 1 << 20),
        name="collect",
    )(wanted, returned)


def add_up_body(parts_ref, out_ref):
    out_ref[...] = jnp.sum(parts_ref[...].astype(F32), axis=0).T


def add_up(parts):
    return pl.pallas_call(
        add_up_body,
        in_specs=[VMEM],
        out_specs=VMEM,
        out_shape=jax.ShapeDtypeStruct(parts.shape[1:], F32),
        cost_estimate=cost(1 << 20, 1 << 20),
        compiler_params=grant(4),
        name="add_up",
    )(parts)


def shards(normed, store, passage_ids, w_query, w_gate, w_key, w_value, cotangent):
    peers = lax.axis_size("st")
    members = lax.axis_size("tp")
    chips = members // 2
    pass_dev = store.shape[0] // PLEN
    table, owners = request(passage_ids, pass_dev, peers)
    wanted = lax.all_to_all(table, "st", 0, 0, tiled=True)

    partner = [(t, t ^ 1) for t in range(members)]
    along = [(2 * z + c, 2 * ((z + 1 - 2 * c) % chips) + c) for z in range(chips) for c in range(2)]
    across = [(a, b ^ 1) for a, b in along]

    def move(array, pairs):
        return lax.ppermute(array, "tp", pairs)

    mine = (w_query, w_gate, w_key, w_value)
    projected = project_rows(store, w_key, w_value, 1024).reshape(pass_dev, PLEN, 2 * DH)
    served, wanted = serve(wanted, projected)
    served, mine, normed_later = lax.optimization_barrier((served, mine, normed))
    arrived = lax.all_to_all(served, "st", 0, 0, tiled=True)
    held, gift, later_held, later_gift = pick(chips, mine)
    lent = move(gift, partner)
    later_lent = move(later_gift, partner)
    queries, upstream, slope = project_tokens(normed_later, mine[0], mine[1], cotangent, 256)
    arrived, held, later_held = lax.optimization_barrier((arrived, held, later_held))
    grads = attend(owners, queries, upstream, slope, arrived)

    other = move(grads, partner)
    opposite, reads3, rows3 = spread(FIRST, grads, other, held, lent, FAR)
    opposite = move(opposite, along)
    reads2, rows2, reads1, rows1, reads0, rows0 = spread(
        REST, grads, other, later_held, later_lent, NEAR
    )
    reads = move(join(reads3, opposite, 1), along)
    parts = weight_grad(grads, normed)
    parts = lax.all_to_all(parts, "st", 0, 0, tiled=True)
    rows = move(join(rows3, opposite, 0), along)
    reads = move(join(reads2, reads), along)
    rows = move(join(rows2, rows), along)
    same, cross = part(reads1, reads)
    outgoing = finish_reads(owners, reads0, move(same, along), move(cross, across), peers)
    same, cross = part(rows1, rows)
    grad_rows = finish_rows(rows0, move(same, along), move(cross, across))
    returned = lax.all_to_all(outgoing, "st", 0, 0, tiled=True)
    grad_store = collect(wanted, returned, pass_dev).reshape(pass_dev * PLEN, DH)
    grad_query_weight = add_up(parts)
    return (grad_rows, grad_store, grad_query_weight)


def solution(mesh):
    placed = (
        P("st", None),
        P("st", None),
        P("st", None),
        P(None, "tp"),
        P(None, "tp"),
        P(None, "tp"),
        P(None, "tp"),
        P("st", "tp"),
    )
    return jax.shard_map(
        shards,
        mesh=mesh,
        in_specs=placed,
        out_specs=(P("st", "tp"), P("st", "tp"), P("st", "tp")),
        check_vma=False,
    )
```

```python
import functools

import jax
import jax.numpy as jnp
from jax import lax
from jax.experimental import pallas as pl
from jax.experimental.pallas import tpu as pltpu
from jax.sharding import PartitionSpec as P


DH = 128
BLK = 128
PLEN = 64
BF16 = jnp.bfloat16
F32 = jnp.float32
NEAR = 40
FAR = 16
TOKENS = 40
ATTEND = 8
SERVE = 61
PROJECT = 61
GRAD = 40
PICK = 61

VMEM = pl.BlockSpec(memory_space=pltpu.VMEM)
SMEM = pl.BlockSpec(memory_space=pltpu.SMEM)


def nt(a, b):
    return lax.dot_general(a, b, (((1,), (1,)), ((), ())), preferred_element_type=F32)


def tn(a, b):
    return lax.dot_general(a, b, (((0,), (0,)), ((), ())), preferred_element_type=F32)


def nn(a, b):
    return lax.dot_general(a, b, (((1,), (0,)), ((), ())), preferred_element_type=F32)


def grant(mib):
    return pltpu.CompilerParams(vmem_limit_bytes=mib << 20)


def cost(flops, nbytes):
    return pl.CostEstimate(flops=flops, bytes_accessed=nbytes, transcendentals=0)


def request_body(pass_dev, ids_ref, table_ref, owner_ref):
    reads, blocks = ids_ref.shape
    lanes = table_ref.shape[1:]
    table_ref[...] = jnp.full(table_ref.shape, -1, jnp.int32)
    for b in range(blocks):
        for r in range(reads):
            passage = ids_ref[r, b]
            owner = lax.div(passage, pass_dev)
            table_ref[owner] = jnp.full(lanes, passage - owner * pass_dev, jnp.int32)
            owner_ref[b * reads + r] = owner


def request(passage_ids, pass_dev, peers):
    return pl.pallas_call(
        functools.partial(request_body, pass_dev),
        in_specs=[SMEM],
        out_specs=[VMEM, SMEM],
        out_shape=[
            jax.ShapeDtypeStruct((peers, 1, 128), jnp.int32),
            jax.ShapeDtypeStruct((passage_ids.size,), jnp.int32),
        ],
        cost_estimate=cost(1 << 16, 1 << 16),
        name="request",
    )(passage_ids.T)


def project_body(x_ref, wa_ref, wb_ref, out_ref):
    pair = jnp.concatenate([wa_ref[...], wb_ref[...]], axis=1)
    out_ref[...] = nn(x_ref[...], pair).astype(BF16)


def project_rows(store, w_key, w_value, tile):
    rows, width = store.shape
    cols = w_key.shape[1]
    return pl.pallas_call(
        project_body,
        grid=(rows // tile,),
        in_specs=[
            pl.BlockSpec((tile, width), lambda i: (i, 0)),
            pl.BlockSpec((width, cols), lambda i: (0, 0)),
            pl.BlockSpec((width, cols), lambda i: (0, 0)),
        ],
        out_specs=pl.BlockSpec((tile, 2 * cols), lambda i: (i, 0)),
        out_shape=jax.ShapeDtypeStruct((rows, 2 * cols), BF16),
        compiler_params=grant(PROJECT),
        cost_estimate=cost(4 * rows * width * cols, 2 * rows * width),
        name="project_store",
    )(store, w_key, w_value)


def serve_body(wanted_ref, rows_ref, out_ref, kept_ref):
    last = rows_ref.shape[0] - 1
    for s in range(out_ref.shape[0]):
        kept_ref[s] = wanted_ref[s, 0, 0]
        out_ref[s] = rows_ref[jnp.clip(wanted_ref[s, 0, 0], 0, last)]


def serve(wanted, projected):
    peers = wanted.shape[0]
    return pl.pallas_call(
        serve_body,
        in_specs=[SMEM, VMEM],
        out_specs=[VMEM, SMEM],
        out_shape=[
            jax.ShapeDtypeStruct((peers,) + projected.shape[1:], BF16),
            jax.ShapeDtypeStruct((peers,), jnp.int32),
        ],
        compiler_params=grant(SERVE),
        cost_estimate=cost(1 << 20, 2 << 20),
        name="serve",
    )(wanted, projected)


def query_body(x_ref, wa_ref, wb_ref, cot_ref, q_ref, up_ref, slope_ref):
    cols = wa_ref.shape[1]
    pair = jnp.concatenate([wa_ref[...], wb_ref[...]], axis=1)
    both = nn(x_ref[...], pair)
    q_ref[...] = both[:, :cols].astype(BF16)
    gate = jax.nn.sigmoid(both[:, cols:])
    up = cot_ref[...].astype(F32) * gate
    up_ref[...] = up.astype(BF16)
    slope_ref[...] = (up * (1.0 - gate)).astype(BF16)


def project_tokens(normed, w_query, w_gate, cotangent, tile):
    rows, width = normed.shape
    cols = w_query.shape[1]
    return pl.pallas_call(
        query_body,
        grid=(rows // tile,),
        in_specs=[
            pl.BlockSpec((tile, width), lambda i: (i, 0)),
            pl.BlockSpec((width, cols), lambda i: (0, 0)),
            pl.BlockSpec((width, cols), lambda i: (0, 0)),
            pl.BlockSpec((tile, cols), lambda i: (i, 0)),
        ],
        out_specs=[pl.BlockSpec((tile, cols), lambda i: (i, 0))] * 3,
        out_shape=[jax.ShapeDtypeStruct((rows, cols), BF16)] * 3,
        compiler_params=grant(TOKENS),
        cost_estimate=cost(4 * rows * width * cols, 2 * rows * width),
        name="project_tokens",
    )(normed, w_query, w_gate, cotangent)


def attend_body(owner_ref, q_ref, up_ref, slope_ref, kv_ref, out_ref):
    scale = DH ** (-0.5)
    tokens = q_ref.shape[0]
    reads = BLK // PLEN
    blocks = range(tokens // BLK)
    rows = [slice(b * BLK, (b + 1) * BLK) for b in blocks]
    kv = [
        jnp.concatenate([kv_ref[owner_ref[reads * b + r]] for r in range(reads)], axis=0)
        for b in blocks
    ]
    scores = [nt(q_ref[rows[b], :], kv[b][:, :DH]) * scale for b in blocks]
    d_att = [up_ref[rows[b], :] for b in blocks]
    d_probs = [nt(d_att[b], kv[b][:, DH:]) for b in blocks]
    grown = [jnp.exp(x - jnp.max(x, axis=1, keepdims=True)) for x in scores]
    probs = [x / jnp.sum(x, axis=1, keepdims=True) for x in grown]
    low = [x.astype(BF16) for x in probs]
    attended = [nn(low[b], kv[b][:, DH:]) for b in blocks]
    delta = [jnp.sum(d_probs[b] * probs[b], axis=1, keepdims=True) for b in blocks]
    d_scores = [(probs[b] * (d_probs[b] - delta[b]) * scale).astype(BF16) for b in blocks]
    for b in blocks:
        at = slice(tokens + b * BLK, tokens + (b + 1) * BLK)
        out_ref[at, DH:] = tn(low[b], d_att[b]).astype(BF16)
    for b in blocks:
        out_ref[rows[b], :DH] = nn(d_scores[b], kv[b][:, :DH]).astype(BF16)
    for b in blocks:
        out_ref[rows[b], DH:] = (slope_ref[rows[b], :].astype(F32) * attended[b]).astype(BF16)
    for b in blocks:
        at = slice(tokens + b * BLK, tokens + (b + 1) * BLK)
        out_ref[at, :DH] = tn(d_scores[b], q_ref[rows[b], :]).astype(BF16)


def attend(owners, queries, upstream, slope, arrived):
    tokens = queries.shape[0]
    return pl.pallas_call(
        attend_body,
        in_specs=[SMEM, VMEM, VMEM, VMEM, VMEM],
        out_specs=VMEM,
        out_shape=jax.ShapeDtypeStruct((2 * tokens, 2 * DH), BF16),
        cost_estimate=cost(14 * tokens * DH * DH, 1 << 20),
        compiler_params=grant(ATTEND),
        name="attend",
    )(owners, queries, upstream, slope, arrived)


def weight_grad_body(d_ref, x_ref, out_ref):
    flipped = d_ref[: x_ref.shape[0], :DH].astype(F32).T.astype(BF16)
    for j in range(out_ref.shape[0] // 2):
        both = nn(flipped, x_ref[:, 2 * j * DH : 2 * (j + 1) * DH]).astype(BF16)
        out_ref[2 * j] = both[:, :DH]
        out_ref[2 * j + 1] = both[:, DH:]


def weight_grad(grads, normed):
    tokens, width = normed.shape
    return pl.pallas_call(
        weight_grad_body,
        in_specs=[VMEM, VMEM],
        out_specs=VMEM,
        out_shape=jax.ShapeDtypeStruct((width // DH, DH, DH), BF16),
        compiler_params=grant(GRAD),
        cost_estimate=cost(2 * tokens * width * DH, 2 * tokens * width),
        name="weight_grad",
    )(grads, normed)


def both_heads(mine_ref, other_ref, side):
    return jnp.concatenate([mine_ref[side, :], other_ref[side, :]], axis=1)


def first_row(chip, core, k, chips):
    to = lax.rem(chip + k + core * (chips - 2 * k), chips)
    return pl.multiple_of(to * 2 * DH, 2 * DH)


FIRST = ((None, 4), (1, 3), (0, 3))
REST = ((1, 2), (0, 2), (1, 1), (0, 1), (1, 0), (0, 0))


def pick_body(chips, *refs):
    weights, outs, sems = refs[:4], refs[4:8], refs[8:]
    at = lax.axis_index("tp")
    here = lax.rem(at, 2)
    chip = lax.div(at, 2)
    jobs = [(n, job) for n, table in enumerate((FIRST, REST)) for job in range(len(table))]

    def copy(n, job, who, piece, half):
        k = (FIRST, REST)[n][job][1]
        core = here if who == 0 else 1 - here
        home = pl.multiple_of((2 * chip + core) * DH, DH)
        start, count = (first_row(chip, core, k, chips), 2 * DH) if k else (home, DH)
        return pltpu.make_async_copy(
            weights[2 * half + piece].at[pl.ds(start, count), :],
            outs[2 * n + who].at[job, pl.ds(0, count), pl.ds(piece * DH, DH)],
            sems[n].at[who, piece, job],
        )

    for n, job in jobs:
        for who in range(2):
            for piece in range(2):
                half = (FIRST, REST)[n][job][0]
                if half is not None:
                    copy(n, job, who, piece, half).start()
                    continue
                for half in range(2):

                    @pl.when(here == (half if who == 0 else 1 - half))
                    def _():
                        copy(n, job, who, piece, half).start()

    for n, job in jobs:
        for who in range(2):
            for piece in range(2):
                copy(n, job, who, piece, 0).wait()


def pick(chips, weights):
    shapes = [
        jax.ShapeDtypeStruct((len(table), 2 * DH, 2 * DH), BF16) for table in (FIRST, REST)
    ]
    return pl.pallas_call(
        functools.partial(pick_body, chips),
        in_specs=[pl.BlockSpec(memory_space=pltpu.HBM)] * 4,
        out_specs=[VMEM] * 4,
        out_shape=[shapes[0], shapes[0], shapes[1], shapes[1]],
        scratch_shapes=[pltpu.SemaphoreType.DMA((2, 2, len(table))) for table in (FIRST, REST)],
        compiler_params=grant(PICK),
        cost_estimate=cost(1 << 28, 6 << 20),
        name="pick",
    )(*weights)


def spread_body(table, mine_ref, other_ref, held_ref, lent_ref, *outs):
    core = lax.rem(lax.axis_index("tp"), 2)
    tokens = mine_ref.shape[0] // 2
    for job, (half, k) in enumerate(table):
        start = core * tokens if half is None else half * tokens
        side = pl.ds(pl.multiple_of(start, tokens), tokens)
        count = 2 * DH if k else DH
        right = jnp.concatenate([held_ref[job, :count, :], lent_ref[job, :count, :]], axis=1)
        outs[job][...] = nt(both_heads(mine_ref, other_ref, side), right).astype(BF16)


def spread(table, mine, other, held, lent, mib):
    tokens = mine.shape[0] // 2
    return pl.pallas_call(
        functools.partial(spread_body, table),
        in_specs=[VMEM] * 4,
        out_specs=[VMEM] * len(table),
        out_shape=[
            jax.ShapeDtypeStruct((tokens, 2 * DH if k else DH), BF16) for _, k in table
        ],
        compiler_params=grant(mib),
        cost_estimate=cost(16 * len(table) * tokens * DH * DH, 2 << 20),
    )(mine, other, held, lent)


def join_body(chosen, own_ref, came_ref, out_ref):
    came = came_ref[...].astype(F32)
    if chosen is not None:
        core = lax.rem(lax.axis_index("tp"), 2)
        came = jnp.where(core == chosen, came, jnp.zeros_like(came))
    out_ref[...] = (own_ref[...].astype(F32) + came).astype(BF16)


def join(own, came, chosen=None):
    return pl.pallas_call(
        functools.partial(join_body, chosen),
        in_specs=[VMEM] * 2,
        out_specs=VMEM,
        out_shape=jax.ShapeDtypeStruct(own.shape, BF16),
        compiler_params=grant(4),
        cost_estimate=cost(1 << 20, 1 << 20),
    )(own, came)


def part_body(own_ref, came_ref, same_ref, cross_ref):
    both = own_ref[...].astype(F32) + came_ref[...].astype(F32)
    core = lax.rem(lax.axis_index("tp"), 2)
    same_ref[...] = jnp.where(core == 0, both[:, :DH], both[:, DH:]).astype(BF16)
    cross_ref[...] = jnp.where(core == 0, both[:, DH:], both[:, :DH]).astype(BF16)


def part(own, came):
    return pl.pallas_call(
        part_body,
        in_specs=[VMEM] * 2,
        out_specs=[VMEM] * 2,
        out_shape=[jax.ShapeDtypeStruct((own.shape[0], DH), BF16)] * 2,
        compiler_params=grant(4),
        cost_estimate=cost(1 << 20, 1 << 20),
    )(own, came)


def total(own_ref, ours_ref, theirs_ref, at):
    return own_ref[at, :].astype(F32) + ours_ref[at, :].astype(F32) + theirs_ref[at, :].astype(F32)


def finish_reads_body(owner_ref, own_ref, ours_ref, theirs_ref, slots_ref):
    slots_ref[...] = jnp.zeros_like(slots_ref)
    for i in range(own_ref.shape[0] // PLEN):
        at = slice(i * PLEN, (i + 1) * PLEN)
        slots_ref[owner_ref[i]] = total(own_ref, ours_ref, theirs_ref, at).astype(BF16)


def finish_reads(owners, own, ours, theirs, peers):
    return pl.pallas_call(
        finish_reads_body,
        in_specs=[SMEM, VMEM, VMEM, VMEM],
        out_specs=VMEM,
        out_shape=jax.ShapeDtypeStruct((peers, PLEN, DH), BF16),
        compiler_params=grant(8),
        cost_estimate=cost(1 << 20, 1 << 20),
        name="finish_reads",
    )(owners, own, ours, theirs)


def finish_rows_body(own_ref, ours_ref, theirs_ref, out_ref):
    out_ref[...] = total(own_ref, ours_ref, theirs_ref, slice(0, own_ref.shape[0]))


def finish_rows(own, ours, theirs):
    return pl.pallas_call(
        finish_rows_body,
        in_specs=[VMEM] * 3,
        out_specs=VMEM,
        out_shape=jax.ShapeDtypeStruct(own.shape, F32),
        compiler_params=grant(8),
        cost_estimate=cost(1 << 20, 1 << 20),
        name="finish_rows",
    )(own, ours, theirs)


def collect_body(wanted_ref, returned_ref, out_ref):
    out_ref[...] = jnp.zeros_like(out_ref)
    for s in range(returned_ref.shape[0]):

        @pl.when(wanted_ref[s] >= 0)
        def _():
            at = jnp.clip(wanted_ref[s], 0, out_ref.shape[0] - 1)
            out_ref[at] = out_ref[at] + returned_ref[s].astype(F32)


def collect(wanted, returned, passages):
    return pl.pallas_call(
        collect_body,
        in_specs=[SMEM, VMEM],
        out_specs=VMEM,
        out_shape=jax.ShapeDtypeStruct((passages, PLEN, DH), F32),
        compiler_params=grant(8),
        cost_estimate=cost(1 << 20, 1 << 20),
        name="collect",
    )(wanted, returned)


def add_up_body(parts_ref, out_ref):
    out_ref[...] = jnp.sum(parts_ref[...].astype(F32), axis=0).T


def add_up(parts):
    return pl.pallas_call(
        add_up_body,
        in_specs=[VMEM],
        out_specs=VMEM,
        out_shape=jax.ShapeDtypeStruct(parts.shape[1:], F32),
        cost_estimate=cost(1 << 20, 1 << 20),
        compiler_params=grant(4),
        name="add_up",
    )(parts)


def shards(normed, store, passage_ids, w_query, w_gate, w_key, w_value, cotangent):
    peers = lax.axis_size("st")
    members = lax.axis_size("tp")
    chips = members // 2
    pass_dev = store.shape[0] // PLEN
    table, owners = request(passage_ids, pass_dev, peers)
    wanted = lax.all_to_all(table, "st", 0, 0, tiled=True)

    partner = [(t, t ^ 1) for t in range(members)]
    along = [(2 * z + c, 2 * ((z + 1 - 2 * c) % chips) + c) for z in range(chips) for c in range(2)]
    across = [(a, b ^ 1) for a, b in along]

    def move(array, pairs):
        return lax.ppermute(array, "tp", pairs)

    mine = (w_query, w_gate, w_key, w_value)
    projected = project_rows(store, w_key, w_value, 1024).reshape(pass_dev, PLEN, 2 * DH)
    served, wanted = serve(wanted, projected)
    served, mine, normed_later = lax.optimization_barrier((served, mine, normed))
    arrived = lax.all_to_all(served, "st", 0, 0, tiled=True)
    held, gift, later_held, later_gift = pick(chips, mine)
    lent = move(gift, partner)
    later_lent = move(later_gift, partner)
    queries, upstream, slope = project_tokens(normed_later, mine[0], mine[1], cotangent, 256)
    arrived, held, later_held = lax.optimization_barrier((arrived, held, later_held))
    grads = attend(owners, queries, upstream, slope, arrived)

    other = move(grads, partner)
    opposite, reads3, rows3 = spread(FIRST, grads, other, held, lent, FAR)
    opposite = move(opposite, along)
    reads2, rows2, reads1, rows1, reads0, rows0 = spread(
        REST, grads, other, later_held, later_lent, NEAR
    )
    reads = move(join(reads3, opposite, 1), along)
    parts = weight_grad(grads, normed)
    parts = lax.all_to_all(parts, "st", 0, 0, tiled=True)
    rows = move(join(rows3, opposite, 0), along)
    reads = move(join(reads2, reads), along)
    rows = move(join(rows2, rows), along)
    same, cross = part(reads1, reads)
    outgoing = finish_reads(owners, reads0, move(same, along), move(cross, across), peers)
    same, cross = part(rows1, rows)
    grad_rows = finish_rows(rows0, move(same, along), move(cross, across))
    returned = lax.all_to_all(outgoing, "st", 0, 0, tiled=True)
    grad_store = collect(wanted, returned, pass_dev).reshape(pass_dev * PLEN, DH)
    grad_query_weight = add_up(parts)
    return (grad_rows, grad_store, grad_query_weight)


def solution(mesh):
    placed = (
        P("st", None),
        P("st", None),
        P("st", None),
        P(None, "tp"),
        P(None, "tp"),
        P(None, "tp"),
        P(None, "tp"),
        P("st", "tp"),
    )
    return jax.shard_map(
        shards,
        mesh=mesh,
        in_specs=placed,
        out_specs=(P("st", "tp"), P("st", "tp"), P("st", "tp")),
        check_vma=False,
    )
```
